32 devices in a mesh: sp: 4 (over y, x), tp: 8 (over z, core).
Axes of the slice: x: 2, y: 2, z: 4, core: 2. Of those that a mesh axis runs over, the one named last changes fastest.
Arguments:
- moe_input: bfloat16 [512, 2048], P('sp'), may hold values from -6 to 6
- cotangent: bfloat16 [512, 2048], P('sp'), may hold values from -6 to 6
- route_expert: int32 [512, 2], P('sp'), may hold values from 0 to 3, all different within a row; in each aligned block of 128 rows (0 to 127, 128 to 255, ...) at most 128 rows name the same one
- route_weight: float32 [512, 2], P('sp'), may hold values from 0.2 to 1
- w_gate: bfloat16 [4, 2048, 6144], P('sp', None, 'tp'), may hold values from -0.125 to 0.125
- w_up: bfloat16 [4, 2048, 6144], P('sp', None, 'tp'), may hold values from -0.125 to 0.125
- w_down: bfloat16 [4, 6144, 2048], P('sp', 'tp'), may hold values from -0.078125 to 0.078125
- out_proj: bfloat16 [2048, 2048], P('tp'), may hold values from -0.125 to 0.125
- saved_out: bfloat16 [512, 2048], P('sp', 'tp'), may hold values from -6 to 6
- queries: bfloat16 [512, 1024], P('sp', 'tp'), may hold values from -6 to 6
- keys: bfloat16 [512, 1024], P('sp', 'tp'), may hold values from -6 to 6
- values: bfloat16 [512, 2048], P('sp', 'tp'), may hold values from -6 to 6
- log_decay: float32 [512, 1024], P('sp', 'tp'), may hold values from -1 to 0
- span_state: float32 [8, 1024, 128], P('sp', 'tp'), may hold values from -6 to 6
Outputs:
- grad_w_gate: bfloat16 [4, 2048, 6144], P('sp', None, 'tp')
- grad_w_up: bfloat16 [4, 2048, 6144], P('sp', None, 'tp')
- grad_w_down: bfloat16 [4, 6144, 2048], P('sp', 'tp')
- grad_proj: float32 [2048, 2048], P('sp', 'tp')
- grad_queries: bfloat16 [512, 1024], P('sp', 'tp')
- grad_keys: bfloat16 [512, 1024], P('sp', 'tp')
- grad_values: bfloat16 [512, 2048], P('sp', 'tp')
- grad_decay: float32 [512, 1024], P('sp', 'tp')
The draws below stay inside these ranges and needn't reach their ends.
Inputs may be any that keep to these rules, and one draw needn't show every extreme that they name: `route_expert`: each row names two different experts. Within the 128 rows of one index of sp no expert is named by more than 128 rows, a bound that some block reaches.
All inputs are finite; a program needn't handle non-finite values.
Results may differ from the reference program's by a relative error of at most 0.019.
Values may be sent and summed in bfloat16 or wider, within the bound.
A program may use at most 128 MiB of HBM per device.

```python
import math
import jax
import jax.numpy as jnp
import numpy as np
from jax import lax

D = 2048
HEADS = 16
DK = 64
DV = 128
F = 6144
SPAN = 64
TOK_DEV = 128
TOKENS = 512
EXPERTS = 4
CAP = 128
N_SP = 4


def draw_log_decay(key, part):
    keys_list = jax.random.split(jax.random.fold_in(key, 11), 7)
    channels = HEADS * DK
    fast_variant = jax.random.uniform(keys_list[0], (channels,)) < 0.5
    slow_rate = jnp.log(10.0) / TOKENS * jax.random.uniform(keys_list[1], (channels,), minval=0.1, maxval=0.4)
    quick_rate = 1.0 / jax.random.uniform(keys_list[2], (channels,), minval=30.0, maxval=50.0)
    starting_offset = jnp.where(fast_variant, quick_rate, slow_rate)
    coarse_estimate = jnp.exp(jax.random.uniform(keys_list[3], (TOKENS, channels), minval=-0.7, maxval=0.7))
    levels = jax.random.uniform(keys_list[4], (TOKENS // TOK_DEV, 1, 1), minval=-0.7, maxval=0.7)
    block_multiplier = jnp.exp(jnp.broadcast_to(levels, (TOKENS // TOK_DEV, TOK_DEV, 1)).reshape(TOKENS, 1))
    target_locations = jax.random.randint(keys_list[5], (3,), 0, TOKENS)
    token_locations = jnp.arange(TOKENS, dtype=jnp.int32)
    transfer_group_rows = jnp.any(token_locations[:, None] == target_locations[None, :], axis=1).astype(jnp.float32)
    layer_stack_depth = -jnp.log(jax.random.uniform(keys_list[6], (channels,), minval=0.5, maxval=0.8))
    transfer_group = transfer_group_rows[:, None] * jnp.where(fast_variant, 0.0, layer_stack_depth)[None, :]
    return (-(starting_offset[None, :] * coarse_estimate * block_multiplier) - transfer_group).astype(jnp.float32)


def raised(values, rng, source, target, shards_of, factor):
    owner, partner = [(jnp.arange(values.shape[position]) // (values.shape[position] // shards_of)).reshape([-1 if axis == position else 1 for axis in range(values.ndim)]) for position in (source, target)]
    chosen = jax.random.permutation(rng, shards_of)[partner]
    strong = (owner == chosen) | (owner == (partner + shards_of // 2) % shards_of)
    return jnp.where(strong, factor * values, values)


def shard_levels(stream_key, dims, cuts, low, top_value):
    gain, own = 1.0, jax.random.fold_in(stream_key, 6)
    for position, blocks in cuts:
        heights = jnp.exp(jax.random.uniform(jax.random.fold_in(own, position), (blocks,), jnp.float32, low / len(cuts), top_value / len(cuts)))
        gain = gain * jnp.repeat(heights, dims[position] // blocks).reshape([-1 if axis == position else 1 for axis in range(len(dims))])
    return gain


def routed_block(own_key, own, number, rows, count, top, limit, slope):
    ranking = jax.random.permutation(own_key, count)
    crowded, ordinary = portions_of(count, rows * top, limit, slope, True), portions_of(count, rows * top, limit, slope, False)
    places = jnp.arange(count)

    def named(lengths, offset_by):
        used = int((lengths > 0).sum())
        fixed = max(1, used // 4)
        moved = fixed + (places - fixed + offset_by * (used - fixed)) % max(1, count - fixed)
        return jnp.zeros((count,), jnp.int32).at[ranking[jnp.where(places < fixed, places, moved)]].set(jnp.asarray(lengths, jnp.int32))

    lengths = jnp.where(number % 4 == 0, named(crowded, number // 4), named(ordinary, number - number // 4 - 1))
    mixed = jax.random.permutation(jax.random.fold_in(own, 3), count)
    source_of, taker = mixed[0:count // 2 * 2:2], mixed[1:count // 2 * 2:2]
    room = jnp.minimum(lengths[source_of] - 1, limit - lengths[taker]) // 2
    room = jnp.where((source_of == ranking[0]) | (taker == ranking[0]) | (lengths[taker] == 0), 0, jnp.maximum(room, 0))
    moved = jax.random.randint(jax.random.fold_in(own, 4), (count // 2,), 0, 1 << 20) % (room + 1)
    lengths = lengths.at[source_of].add(-moved).at[taker].add(moved)
    items = jnp.searchsorted(jnp.cumsum(lengths), jnp.arange(rows * top), side="right").astype(jnp.int32)
    table = items.reshape(top, rows).T
    table = table[jax.random.permutation(jax.random.fold_in(own, 1), rows)]
    offset_by = jax.random.randint(jax.random.fold_in(own, 2), (rows, 1), 0, top)
    return jnp.take_along_axis(table, (jnp.arange(top)[None, :] + offset_by) % top, axis=1)


def portions_of(count, total, bound, lean, full):
    loads = [(1 << 20) // math.isqrt(standing ** lean) + 1 for standing in range(1, count + 1)]
    largest = bound if full else min(bound, max(-(-total // count), total * loads[0] // sum(loads)))
    least = 1 if total - largest >= count - 1 else 0
    holding, spare = [largest] + [least] * (count - 1), total - largest - least * (count - 1)
    while spare > 0:
        free = [i for i in range(1, count) if holding[i] < largest] or [i for i in range(1, count) if holding[i] < bound]
        whole, left = sum([loads[i] for i in free]), spare
        for i in free:
            extra = min(bound - holding[i], max(1, left * loads[i] // whole), spare)
            holding[i] = holding[i] + extra
            spare = spare - extra
    return np.array(holding)


def normal_values(rng, extent, spread, most, shards=(), kind=jnp.bfloat16):
    drawn = spread * jax.random.normal(rng, extent, jnp.float32)
    if shards:
        drawn = drawn * shard_levels(rng, extent, shards, -0.22, 0.18)
    return jnp.clip(drawn, -most, most).astype(kind)


def bell_draw_with(own_key, shape, scale, most, cuts, heavy, held_as=jnp.bfloat16):
    values = scale * jax.random.normal(own_key, shape, jnp.float32)
    if cuts:
        values = values * shard_levels(own_key, shape, cuts, -0.22, 0.18)
    return jnp.clip(raised(values, jax.random.fold_in(own_key, 3), *heavy), -most, most).astype(held_as)


def setup_inputs(seed: int = 0) -> dict:
    seeds = jax.random.split(jax.random.key(seed), 15)
    moe_input = normal_values(seeds[0], (TOKENS, D), 1.0, 6.0, ((0, 4),))
    cotangent = bell_draw_with(seeds[1], (TOKENS, D), 1.0, 6.0, ((0, 4),), (0, 1, 4, 2.0))
    route_expert_keys = jax.random.split(jax.random.fold_in(seeds[2], 1), TOKENS // TOK_DEV)
    route_expert_turns = jax.random.permutation(jax.random.fold_in(seeds[2], 3), TOKENS // TOK_DEV)
    route_expert = jax.vmap(lambda own, number: routed_block(jax.random.fold_in(seeds[2], 2), own, number, TOK_DEV, EXPERTS, 2, CAP, 1))(route_expert_keys, route_expert_turns).reshape((TOKENS, 2))
    route_weight = jnp.clip(0.2 + 0.8 * jax.random.uniform(seeds[3], (TOKENS, 2), jnp.float32) ** shard_levels(seeds[3], (TOKENS, 2), ((0, 4),), -0.2, 0.2), 0.2, 1.0)
    w_gate = normal_values(seeds[4], (EXPERTS, D, F), D ** -0.5, 0.125, ((0, 4), (2, 8)))
    w_up = normal_values(seeds[5], (EXPERTS, D, F), D ** -0.5, 0.125, ((0, 4), (2, 8)))
    w_down = normal_values(seeds[6], (EXPERTS, F, D), F ** -0.5, 0.078125, ((0, 4), (1, 8)))
    out_proj = normal_values(seeds[7], (HEADS * DV, D), (HEADS * DV) ** -0.5, 0.125, ((0, 8),))
    saved_out = normal_values(seeds[8], (TOKENS, HEADS * DV), 1.0, 6.0, ((0, 4), (1, 8)))
    queries = normal_values(seeds[9], (TOKENS, HEADS * DK), 1.0, 6.0, ((0, 4), (1, 8)))
    keys = normal_values(seeds[10], (TOKENS, HEADS * DK), 1.0, 6.0, ((0, 4), (1, 8)))
    values = normal_values(seeds[11], (TOKENS, HEADS * DV), 1.0, 6.0, ((0, 4), (1, 8)))
    log_decay = draw_log_decay(jax.random.fold_in(seeds[14], 71), 0)
    span_state = normal_values(seeds[13], (TOKENS // SPAN, HEADS * DK, DV), 1.0, 6.0, ((0, 4), (1, 8)), jnp.float32)
    return {"moe_input": moe_input, "cotangent": cotangent, "route_expert": route_expert, "route_weight": route_weight, "w_gate": w_gate, "w_up": w_up, "w_down": w_down, "out_proj": out_proj, "saved_out": saved_out, "queries": queries, "keys": keys, "values": values, "log_decay": log_decay, "span_state": span_state}


HIGH = lax.Precision.HIGHEST

def slot_places(experts, count):
    routes_flat = experts.reshape(-1)
    one_hot = (routes_flat[:, None] == jnp.arange(count, dtype=jnp.int32)[None, :]).astype(jnp.int32)
    earlier = jnp.cumsum(one_hot, axis=0) - one_hot
    return lax.optimization_barrier(jnp.sum(earlier * one_hot, axis=1)).reshape(experts.shape).astype(jnp.int32)

def expert_grads(inputs, routed, gate_weight, up_weight, down_weight):
    gate = jnp.dot(inputs, gate_weight, preferred_element_type=jnp.float32)
    upper = jnp.dot(inputs, up_weight, preferred_element_type=jnp.float32)
    sigmoid_gate = jax.nn.sigmoid(gate)
    active = gate * sigmoid_gate
    hidden = (active * upper).astype(jnp.bfloat16)
    d_hidden = lax.dot_general(routed, down_weight, (((1,), (1,)), ((), ())), preferred_element_type=jnp.float32)
    d_upper = (d_hidden * active).astype(jnp.bfloat16)
    d_gate = (d_hidden * upper * sigmoid_gate * (1.0 + gate * (1.0 - sigmoid_gate))).astype(jnp.bfloat16)
    grad_down = lax.dot_general(hidden, routed, (((0,), (0,)), ((), ())), preferred_element_type=jnp.float32).astype(jnp.bfloat16)
    grad_gate = lax.dot_general(inputs, d_gate, (((0,), (0,)), ((), ())), preferred_element_type=jnp.float32).astype(jnp.bfloat16)
    grad_up = lax.dot_general(inputs, d_upper, (((0,), (0,)), ((), ())), preferred_element_type=jnp.float32).astype(jnp.bfloat16)
    return (d_gate, d_upper, grad_gate, grad_up, grad_down)

def input_grad(d_gate, d_upper, gate_weight, up_weight):
    first = lax.dot_general(d_gate, gate_weight, (((1,), (1,)), ((), ())), preferred_element_type=jnp.float32)
    second = lax.dot_general(d_upper, up_weight, (((1,), (1,)), ((), ())), preferred_element_type=jnp.float32)
    return first + second

def gated_pieces(queries, keys, values, log_decay, grad_mix, key_dim, span_len):
    value_dim = values.shape[1] * key_dim // queries.shape[1]
    heads = queries.shape[1] // key_dim
    spans = queries.shape[0] // span_len

    def blocks(array, width):
        return array.astype(jnp.float32).reshape(spans, span_len, heads, width)
    query_spans = blocks(queries, key_dim)
    key_spans = blocks(keys, key_dim)
    value_spans = blocks(values, value_dim)
    grad_spans = blocks(grad_mix, value_dim)
    cumulative = jnp.cumsum(blocks(log_decay, key_dim), axis=1)
    last = cumulative[:, -1]
    scale = key_dim ** (-0.5)
    query_decayed = query_spans * jnp.exp(cumulative)
    key_grown = key_spans * jnp.exp(-cumulative)
    key_to_end = key_spans * jnp.exp(last[:, None] - cumulative)
    g_local = scale * jnp.einsum('nthk,nthv->nhkv', query_decayed, grad_spans, precision=HIGH)
    return (query_spans, key_spans, value_spans, grad_spans, cumulative, last, query_decayed, key_grown, key_to_end, g_local)

def backward_step(carry, inputs):
    local, decay = inputs
    return (local + jnp.exp(decay)[..., None] * carry, carry)

def gated_finish(pieces, span_state, g_end, key_dim):
    query_spans, key_spans, value_spans, grad_spans, cumulative, last, query_decayed, key_grown, key_to_end, g_local = pieces
    spans, span_len, heads, value_dim = value_spans.shape
    scale = key_dim ** (-0.5)
    token_locations = jnp.arange(span_len, dtype=jnp.int32)
    causal = (token_locations[:, None] >= token_locations[None, :]).astype(jnp.float32)
    scores = jnp.einsum('nthk,nshk->nhts', query_decayed, key_grown, precision=HIGH) * causal
    grad_dot = jnp.einsum('nthv,nshv->nhts', grad_spans, value_spans, precision=HIGH) * causal
    state = span_state.astype(jnp.float32).reshape(spans, heads, key_dim, value_dim)
    d_query = scale * jnp.exp(cumulative) * (jnp.einsum('nhts,nshk->nthk', grad_dot, key_grown, precision=HIGH) + jnp.einsum('nthv,nhkv->nthk', grad_spans, state, precision=HIGH))
    d_key = scale * jnp.exp(-cumulative) * jnp.einsum('nhts,nthk->nshk', grad_dot, query_decayed, precision=HIGH) + jnp.exp(last[:, None] - cumulative) * jnp.einsum('nshv,nhkv->nshk', value_spans, g_end, precision=HIGH)
    d_value = scale * jnp.einsum('nhts,nthv->nshv', scores, grad_spans, precision=HIGH) + jnp.einsum('nshk,nhkv->nshv', key_to_end, g_end, precision=HIGH)
    state_end = jnp.exp(last)[..., None] * state + jnp.einsum('nshk,nshv->nhkv', key_to_end, value_spans, precision=HIGH)
    tail = lax.optimization_barrier(jnp.sum(state_end * g_end, axis=-1))
    d_cumulative = query_spans * d_query - key_spans * d_key
    d_log = jnp.cumsum(d_cumulative[:, ::-1], axis=1)[:, ::-1] + tail[:, None]
    rows = spans * span_len
    return (d_query.reshape(rows, heads * key_dim).astype(jnp.bfloat16), d_key.reshape(rows, heads * key_dim).astype(jnp.bfloat16), d_value.reshape(rows, heads * value_dim).astype(jnp.bfloat16), d_log.reshape(rows, heads * key_dim))

def place_block(block):
    return slot_places(block, EXPERTS)

def per_expert(items):
    rows_in, rows_cot, gate_weight, up_weight, down_weight = items
    d_gate, d_upper, grad_gate, grad_up, grad_down = expert_grads(rows_in, rows_cot, gate_weight, up_weight, down_weight)
    return (input_grad(d_gate, d_upper, gate_weight, up_weight), grad_gate, grad_up, grad_down)

def reference(moe_input, cotangent, route_expert, route_weight, w_gate, w_up, w_down, out_proj, saved_out, queries, keys, values, log_decay, span_state):
    blocks = route_expert.reshape(N_SP, TOK_DEV, 2)
    target_locations = jax.vmap(place_block)(blocks)
    source = jnp.arange(N_SP, dtype=jnp.int32)[:, None, None]
    slot_index = (blocks * (N_SP * CAP) + source * CAP + target_locations).reshape(-1).astype(jnp.int32)
    owner = jnp.full((EXPERTS * N_SP * CAP,), 2 * TOKENS, jnp.int32).at[slot_index].set(jnp.arange(2 * TOKENS, dtype=jnp.int32))
    weighted = (route_weight[:, :, None] * cotangent[:, None, :].astype(jnp.float32)).astype(jnp.bfloat16)
    weighted = weighted.reshape(2 * TOKENS, D)
    blank = jnp.zeros((1, D), jnp.bfloat16)
    slot_cot = jnp.concatenate([weighted, blank], axis=0)[owner].reshape(EXPERTS, N_SP * CAP, D)
    slot_in = jnp.concatenate([moe_input, blank], axis=0)[owner // 2].reshape(EXPERTS, N_SP * CAP, D)
    slot_grad, grad_w_gate, grad_w_up, grad_w_down = lax.map(per_expert, (slot_in, slot_cot, w_gate, w_up, w_down))
    routed = slot_grad.reshape(-1, D)[slot_index].reshape(TOKENS, 2, D)
    grad_in = (cotangent.astype(jnp.float32) + routed[:, 0] + routed[:, 1]).astype(jnp.bfloat16)
    grad_mix = lax.dot_general(grad_in, out_proj, (((1,), (1,)), ((), ())), preferred_element_type=jnp.float32)
    grad_proj = lax.dot_general(grad_in, saved_out, (((0,), (0,)), ((), ())), preferred_element_type=jnp.float32)
    pieces = gated_pieces(queries, keys, values, log_decay, grad_mix, DK, SPAN)
    g_local = pieces[9]
    last = pieces[5]
    begin = jnp.zeros((HEADS, DK, DV), jnp.float32)
    ignored, g_end = lax.scan(backward_step, begin, (g_local, last), reverse=True)
    grad_queries, grad_keys, grad_values, grad_decay = gated_finish(pieces, span_state, g_end, DK)
    return (grad_w_gate, grad_w_up, grad_w_down, grad_proj, grad_queries, grad_keys, grad_values, grad_decay)
```

```python
import functools

import jax
import jax.numpy as jnp
from jax import lax
from jax.experimental import pallas as pl
from jax.experimental.pallas import tpu as pltpu
from jax.sharding import PartitionSpec as P

DK = 64
SPAN = 64

HIGH = lax.Precision.HIGHEST
F32 = jnp.float32
BF16 = jnp.bfloat16


def dot(a, b, dims, precision=HIGH):
    return lax.dot_general(
        a, b, ((dims[0], dims[1]), ((), ())), precision=precision, preferred_element_type=F32
    )


NN = ((1,), (0,))
NT = ((1,), (1,))
TN = ((0,), (0,))


def triangle(size, upper):
    row = lax.broadcasted_iota(jnp.int32, (size, size), 0)
    col = lax.broadcasted_iota(jnp.int32, (size, size), 1)
    return ((row <= col) if upper else (row >= col)).astype(F32)


def mix_kernel(grad_in, out_proj, queries, log_decay, mix_out, start_out):
    mix = dot(grad_in[...], out_proj[...], NT, None)
    mix_out[...] = mix
    rows, channels = queries.shape
    heads = channels // DK
    wide = mix.shape[1] // heads
    lower = triangle(SPAN, False)
    ones = jnp.ones((SPAN, wide), F32)
    for h in range(heads):
        keyed = slice(h * DK, (h + 1) * DK)
        carry = None
        for n in reversed(range(rows // SPAN)):
            at = slice(n * SPAN, (n + 1) * SPAN)
            decay = log_decay[at, keyed]
            qd = queries[at, keyed].astype(F32) * jnp.exp(dot(lower, decay, NN))
            local = DK**-0.5 * dot(qd, mix[at, h * wide : (h + 1) * wide], TN)
            if carry is not None:
                local = local + jnp.exp(dot(decay, ones, TN)) * carry
            carry = local
        start_out[keyed, :] = carry


def finish_kernel(queries, keys, values, log_decay, mix, state, after, dq_o, dk_o, dv_o, dl_o):
    rows, channels = queries.shape
    heads = channels // DK
    wide = values.shape[1] // heads
    lower = triangle(SPAN, False)
    upper = triangle(SPAN, True)
    ones = jnp.ones((SPAN, wide), F32)
    scale = DK**-0.5
    for h in range(heads):
        keyed = slice(h * DK, (h + 1) * DK)
        valued = slice(h * wide, (h + 1) * wide)
        g_end = after[keyed, :]
        for n in reversed(range(rows // SPAN)):
            at = slice(n * SPAN, (n + 1) * SPAN)
            q = queries[at, keyed].astype(F32)
            k = keys[at, keyed].astype(F32)
            v = values[at, valued].astype(F32)
            g = mix[at, valued]
            s0 = state[n, keyed, :]
            decay = log_decay[at, keyed]
            c = dot(lower, decay, NN)
            last = c[SPAN - 1 : SPAN, :]
            grow, shrink, to_end = jnp.exp(c), jnp.exp(-c), jnp.exp(last - c)
            qd, kd, ke = q * grow, k * shrink, k * to_end
            scores = dot(qd, kd, NT) * lower
            gv = dot(g, v, NT) * lower
            dq = scale * grow * (dot(gv, kd, NN) + dot(g, s0, NT))
            dk = scale * shrink * dot(gv, qd, TN) + to_end * dot(v, g_end, NT)
            dv = scale * dot(scores, g, TN) + dot(ke, g_end, NN)
            e_last = jnp.exp(dot(decay, ones, TN))
            s1 = e_last * s0 + dot(ke, v, TN)
            dq_o[at, keyed] = dq.astype(BF16)
            dk_o[at, keyed] = dk.astype(BF16)
            dv_o[at, valued] = dv.astype(BF16)
            dl_o[at, keyed] = dot(upper, q * dq - k * dk, NN) + dot(ones, s1 * g_end, NT)
            if n:
                g_end = DK**-0.5 * dot(qd, g, TN) + e_last * g_end


def call(kernel, outs, *args):
    return pl.pallas_call(
        kernel,
        out_shape=[jax.ShapeDtypeStruct(s, d) for s, d in outs],
        in_specs=[pl.BlockSpec(memory_space=pltpu.VMEM)] * len(args),
        out_specs=[pl.BlockSpec(memory_space=pltpu.VMEM)] * len(outs),
        cost_estimate=pl.CostEstimate(flops=2 * 10**8, bytes_accessed=10**6, transcendentals=0),
    )(*args)


def on_device(
    moe_input,
    cotangent,
    route_expert,
    route_weight,
    w_gate,
    w_up,
    w_down,
    out_proj,
    saved_out,
    queries,
    keys,
    values,
    log_decay,
    span_state,
):
    tok_rows, width = moe_input.shape
    groups = lax.axis_size("sp")
    lanes = lax.axis_size("tp")
    me = lax.axis_index("sp")
    lane = lax.axis_index("tp")
    inputs = lax.all_gather(moe_input, "sp", axis=0, tiled=True)
    cots = lax.all_gather(cotangent, "sp", axis=0, tiled=True)
    named = route_expert[:, :, None] == jnp.arange(groups, dtype=jnp.int32)
    weights = jnp.sum(jnp.where(named, route_weight[:, :, None], 0.0), axis=1).T
    small = lax.all_gather(
        jnp.concatenate([weights.reshape(-1), jnp.sum(log_decay, axis=0)]), "sp"
    )
    weights_all = small[:, : groups * tok_rows].reshape(groups, groups, tok_rows)
    mine = lax.dynamic_index_in_dim(weights_all, me, 1, keepdims=False).reshape(-1, 1)
    decays = small[:, groups * tok_rows :]

    gate_weight, up_weight, down_weight = w_gate[0], w_up[0], w_down[0]
    gate = jnp.dot(inputs, gate_weight, preferred_element_type=F32)
    upper = jnp.dot(inputs, up_weight, preferred_element_type=F32)
    routed = (mine * cots.astype(F32)).astype(BF16)
    sigmoid_gate = jax.nn.sigmoid(gate)
    active = gate * sigmoid_gate
    hidden = (active * upper).astype(BF16)
    d_hidden = dot(routed, down_weight, NT, None)
    d_upper = (d_hidden * active).astype(BF16)
    d_gate = (d_hidden * upper * sigmoid_gate * (1.0 + gate * (1.0 - sigmoid_gate))).astype(BF16)
    slots = (dot(d_gate, gate_weight, NT, None) + dot(d_upper, up_weight, NT, None)).astype(BF16)
    part = lax.psum_scatter(slots, ("sp", "tp"), scatter_dimension=0, tiled=True)
    grad_down = dot(hidden, routed, TN, None).astype(BF16)
    grad_gate = dot(inputs, d_gate, TN, None).astype(BF16)
    grad_up = dot(inputs, d_upper, TN, None).astype(BF16)

    share = tok_rows // lanes
    own = lax.dynamic_slice_in_dim(cotangent, lane * share, share, 0)
    part = (own.astype(F32) + part.astype(F32)).astype(BF16)
    grad_in = lax.all_gather(part, "tp", axis=0, tiled=True)

    channels, wide = queries.shape[1], span_state.shape[2]
    mix, start = call(
        mix_kernel,
        [((tok_rows, values.shape[1]), F32), ((channels, wide), F32)],
        grad_in,
        out_proj,
        queries,
        log_decay,
    )
    starts = lax.all_gather(start, "sp")
    grad_proj = lax.psum_scatter(
        dot(grad_in, saved_out, TN, None).astype(BF16), "sp", scatter_dimension=0, tiled=True
    ).astype(F32)
    at = jnp.arange(groups, dtype=jnp.int32)
    between = ((at[None, :] > me) & (at[None, :] < at[:, None])).astype(F32)
    factor = jnp.exp(jnp.sum(between[:, :, None] * decays[None], axis=1))
    factor = jnp.where((at > me)[:, None], factor, 0.0)
    after = jnp.sum(factor[:, :, None] * starts, axis=0)
    grad_queries, grad_keys, grad_values, grad_decay = call(
        finish_kernel,
        [
            (queries.shape, BF16),
            (keys.shape, BF16),
            (values.shape, BF16),
            (log_decay.shape, F32),
        ],
        queries,
        keys,
        values,
        log_decay,
        mix,
        span_state,
        after,
    )
    return (
        grad_gate[None],
        grad_up[None],
        grad_down[None],
        grad_proj,
        grad_queries,
        grad_keys,
        grad_values,
        grad_decay,
    )


def solution(mesh):
    placed = (
        P("sp", None),
        P("sp", None),
        P("sp", None),
        P("sp", None),
        P("sp", None, "tp"),
        P("sp", None, "tp"),
        P("sp", "tp", None),
        P("tp", None),
        P("sp", "tp"),
        P("sp", "tp"),
        P("sp", "tp"),
        P("sp", "tp"),
        P("sp", "tp"),
        P("sp", "tp", None),
    )
    return jax.shard_map(
        on_device,
        mesh=mesh,
        in_specs=placed,
        out_specs=(
            P("sp", None, "tp"),
            P("sp", None, "tp"),
            P("sp", "tp", None),
            P("sp", "tp"),
            P("sp", "tp"),
            P("sp", "tp"),
            P("sp", "tp"),
            P("sp", "tp"),
        ),
        check_vma=False,
    )
```

```python
import functools

import jax
import jax.numpy as jnp
from jax import lax
from jax.experimental import pallas as pl
from jax.experimental.pallas import tpu as pltpu
from jax.sharding import PartitionSpec as P

DK = 64
SPAN = 64

HIGH = lax.Precision.HIGHEST
F32 = jnp.float32
BF16 = jnp.bfloat16


def dot(a, b, dims, precision=HIGH):
    return lax.dot_general(
        a, b, ((dims[0], dims[1]), ((), ())), precision=precision, preferred_element_type=F32
    )


NN = ((1,), (0,))
NT = ((1,), (1,))
TN = ((0,), (0,))


def triangle(size, upper):
    row = lax.broadcasted_iota(jnp.int32, (size, size), 0)
    col = lax.broadcasted_iota(jnp.int32, (size, size), 1)
    return ((row <= col) if upper else (row >= col)).astype(F32)


def there(sp=None, tp=None):
    where = {}
    if sp is not None:
        where["sp"] = sp
    if tp is not None:
        where["tp"] = tp
    return where


def greet(partners):
    barrier = pltpu.get_barrier_semaphore()
    for partner in partners:
        pl.semaphore_signal(
            barrier, inc=1, device_id=partner, device_id_type=pl.DeviceIdType.MESH
        )
    pl.semaphore_wait(barrier, len(partners))


def send(src, dst, sems, slot, partner):
    copy = pltpu.make_async_remote_copy(
        src_ref=src,
        dst_ref=dst,
        send_sem=sems[0].at[slot],
        recv_sem=sems[1].at[slot],
        device_id=partner,
        device_id_type=pl.DeviceIdType.MESH,
    )
    copy.start()
    return copy


def gather_kernel(n, own_a, own_b, weights, decays, all_a, all_b, all_w, all_d, *sems):
    me, lane = lax.axis_index("sp"), lax.axis_index("tp")
    core = lax.rem(lane, 2)
    twin = there(tp=lane + 1 - 2 * core)
    rows = own_a.shape[0]
    half = rows // 2
    peers = [there(sp=lax.rem(me + d, n)) for d in range(1, n)]
    greet(peers + [twin])
    far, near = sems[:2], sems[2:4]
    copies = []
    for t, (own, full) in enumerate([(weights, all_w), (decays, all_d)]):
        for d, peer in enumerate(peers):
            copies.append(send(own, full.at[me], far, t * (n - 1) + d, peer))
    bulk = []
    pieces = pl.ds(pl.multiple_of(core * half, half), half)
    for t, (own, full) in enumerate([(own_a, all_a), (own_b, all_b)]):
        for d, peer in enumerate(peers):
            at = pl.ds(pl.multiple_of(me * rows + core * half, half), half)
            bulk.append(send(own.at[pieces], full.at[at], far, (t + 2) * (n - 1) + d, peer))
    here = pl.ds(pl.multiple_of(me * rows, rows), rows)
    all_a[here, :] = own_a[...]
    all_b[here, :] = own_b[...]
    all_w[me] = weights[...]
    all_d[me] = decays[...]
    for t, full in enumerate([all_a, all_b]):
        for d in range(n - 1):
            slot = t * (n - 1) + d
            bulk[slot].wait_recv()
            source = lax.rem(me + n - 1 - d, n)
            at = pl.ds(pl.multiple_of(source * rows + core * half, half), half)
            copies.append(send(full.at[at], full.at[at], near, slot, twin))
    for copy in bulk:
        copy.wait_send()
    for copy in copies:
        copy.wait()


def sum_kernel(n, slots, cot, out, got_a, sum_a, got_b, sum_b, got_c, *sems):
    me, lane = lax.axis_index("sp"), lax.axis_index("tp")
    core = lax.rem(lane, 2)
    z = lax.div(lane, 2)
    half = got_a.shape[1]
    depth = got_c.shape[0] + 1
    piece = half // depth
    rows = 2 * half
    twin = there(tp=lane + 1 - 2 * core)
    peers = [there(sp=lax.rem(me + d, n)) for d in range(1, n)]
    along = [lax.rem(z + d, depth) for d in range(1, depth)]
    lanes = [there(tp=2 * other + core) for other in along]
    greet(peers + lanes + [twin])
    a, b, c, d_, e = (sems[2 * i : 2 * i + 2] for i in range(5))

    def rows_at(start, size):
        return pl.ds(pl.multiple_of(start, size), size)

    first = [
        send(slots.at[rows_at(k * rows + (1 - core) * half, half)], got_a.at[k], a, k, twin)
        for k in range(n)
    ]
    for k in range(n):
        first[k].wait_recv()
        mine = slots[rows_at(k * rows + core * half, half), :].astype(F32)
        sum_a[k] = (mine + got_a[k].astype(F32)).astype(BF16)
    second = [
        send(sum_a.at[lax.rem(me + d, n)], got_b.at[d - 1], b, d - 1, peers[d - 1])
        for d in range(1, n)
    ]
    total = sum_a[me].astype(F32)
    for d in range(n - 1):
        second[d].wait_recv()
        total = total + got_b[d].astype(F32)
    sum_b[...] = total.astype(BF16)
    third = [
        send(sum_b.at[rows_at(along[d] * piece, piece)], got_c.at[d], c, d, lanes[d])
        for d in range(depth - 1)
    ]
    mine = rows_at(core * half + z * piece, piece)
    total = cot[mine, :].astype(F32) + sum_b[rows_at(z * piece, piece), :].astype(F32)
    for d in range(depth - 1):
        third[d].wait_recv()
        total = total + got_c[d].astype(F32)
    out[mine, :] = total.astype(BF16)
    fourth = [send(out.at[mine], out.at[mine], d_, d, lanes[d]) for d in range(depth - 1)]
    for copy in fourth:
        copy.wait_recv()
    whole = rows_at(core * half, half)
    fifth = send(out.at[whole], out.at[whole], e, 0, twin)
    fifth.wait()
    for copy in first + second + third + fourth:
        copy.wait_send()


def mix_kernel(n, grad_in, out_proj, queries, log_decay, mix_out, starts, *sems):
    me = lax.axis_index("sp")
    peers = [there(sp=lax.rem(me + d, n)) for d in range(1, n)]
    greet(peers)
    mix = dot(grad_in[...], out_proj[...], NT, None)
    mix_out[...] = mix
    rows, channels = queries.shape
    heads = channels // DK
    wide = mix.shape[1] // heads
    lower = triangle(SPAN, False)
    ones = jnp.ones((SPAN, wide), F32)
    for h in range(heads):
        keyed = slice(h * DK, (h + 1) * DK)
        carry = None
        for n_ in reversed(range(rows // SPAN)):
            at = slice(n_ * SPAN, (n_ + 1) * SPAN)
            decay = log_decay[at, keyed]
            qd = queries[at, keyed].astype(F32) * jnp.exp(dot(lower, decay, NN))
            local = DK**-0.5 * dot(qd, mix[at, h * wide : (h + 1) * wide], TN)
            if carry is not None:
                local = local + jnp.exp(dot(decay, ones, TN)) * carry
            carry = local
        starts[me, keyed, :] = carry
    copies = [send(starts.at[me], starts.at[me], sems, d, peers[d]) for d in range(n - 1)]
    for copy in copies:
        copy.wait()


def weight_kernel(inputs, routed, hidden, d_gate, d_upper, gate_o, up_o, down_o):
    gate_o[0] = dot(inputs[...], d_gate[...], TN, None).astype(BF16)
    up_o[0] = dot(inputs[...], d_upper[...], TN, None).astype(BF16)
    down_o[0] = dot(hidden[...], routed[...], TN, None).astype(BF16)


def weight_grads(inputs, routed, hidden, d_gate, d_upper):
    slots, width = inputs.shape
    units = hidden.shape[1]
    tile = width // 8
    moving = pl.BlockSpec((slots, tile), lambda i: (0, i))
    still = pl.BlockSpec((slots, units), lambda i: (0, 0))
    return pl.pallas_call(
        weight_kernel,
        grid=(width // tile,),
        out_shape=[
            jax.ShapeDtypeStruct((1, width, units), BF16),
            jax.ShapeDtypeStruct((1, width, units), BF16),
            jax.ShapeDtypeStruct((1, units, width), BF16),
        ],
        in_specs=[moving, moving, still, still, still],
        out_specs=[
            pl.BlockSpec((1, tile, units), lambda i: (0, i, 0)),
            pl.BlockSpec((1, tile, units), lambda i: (0, i, 0)),
            pl.BlockSpec((1, units, tile), lambda i: (0, 0, i)),
        ],
        cost_estimate=pl.CostEstimate(
            flops=6 * slots * width * units,
            bytes_accessed=6 * width * units,
            transcendentals=0,
        ),
    )(inputs, routed, hidden, d_gate, d_upper)


def finish_kernel(queries, keys, values, log_decay, mix, state, after, dq_o, dk_o, dv_o, dl_o):
    rows, channels = queries.shape
    heads = channels // DK
    wide = values.shape[1] // heads
    lower = triangle(SPAN, False)
    upper = triangle(SPAN, True)
    ones = jnp.ones((SPAN, wide), F32)
    scale = DK**-0.5
    for h in range(heads):
        keyed = slice(h * DK, (h + 1) * DK)
        valued = slice(h * wide, (h + 1) * wide)
        g_end = after[keyed, :]
        for n in reversed(range(rows // SPAN)):
            at = slice(n * SPAN, (n + 1) * SPAN)
            q = queries[at, keyed].astype(F32)
            k = keys[at, keyed].astype(F32)
            v = values[at, valued].astype(F32)
            g = mix[at, valued]
            s0 = state[n, keyed, :]
            decay = log_decay[at, keyed]
            c = dot(lower, decay, NN)
            last = c[SPAN - 1 : SPAN, :]
            grow, shrink, to_end = jnp.exp(c), jnp.exp(-c), jnp.exp(last - c)
            qd, kd, ke = q * grow, k * shrink, k * to_end
            scores = dot(qd, kd, NT) * lower
            gv = dot(g, v, NT) * lower
            dq = scale * grow * (dot(gv, kd, NN) + dot(g, s0, NT))
            dk = scale * shrink * dot(gv, qd, TN) + to_end * dot(v, g_end, NT)
            dv = scale * dot(scores, g, TN) + dot(ke, g_end, NN)
            e_last = jnp.exp(dot(decay, ones, TN))
            s1 = e_last * s0 + dot(ke, v, TN)
            dq_o[at, keyed] = dq.astype(BF16)
            dk_o[at, keyed] = dk.astype(BF16)
            dv_o[at, valued] = dv.astype(BF16)
            dl_o[at, keyed] = dot(upper, q * dq - k * dk, NN) + dot(ones, s1 * g_end, NT)
            if n:
                g_end = DK**-0.5 * dot(qd, g, TN) + e_last * g_end


def call(kernel, outs, *args, scratch=(), sems=(), ident=None):
    semaphores = [pltpu.SemaphoreType.DMA((count,)) for count in sems for _ in range(2)]
    return pl.pallas_call(
        kernel,
        out_shape=[jax.ShapeDtypeStruct(s, d) for s, d in outs],
        in_specs=[pl.BlockSpec(memory_space=pltpu.VMEM)] * len(args),
        out_specs=[pl.BlockSpec(memory_space=pltpu.VMEM)] * len(outs),
        scratch_shapes=[pltpu.VMEM(s, BF16) for s in scratch] + semaphores,
        cost_estimate=pl.CostEstimate(flops=2 * 10**8, bytes_accessed=10**6, transcendentals=0),
        compiler_params=pltpu.CompilerParams(
            collective_id=ident, has_side_effects=ident is not None
        ),
    )(*args)


def on_device(
    moe_input,
    cotangent,
    route_expert,
    route_weight,
    w_gate,
    w_up,
    w_down,
    out_proj,
    saved_out,
    queries,
    keys,
    values,
    log_decay,
    span_state,
):
    tok_rows, width = moe_input.shape
    groups = lax.axis_size("sp")
    lanes = lax.axis_size("tp")
    me = lax.axis_index("sp")
    named = route_expert[:, :, None] == jnp.arange(groups, dtype=jnp.int32)
    weights = jnp.sum(jnp.where(named, route_weight[:, :, None], 0.0), axis=1).T
    decay_sum = jnp.sum(log_decay, axis=0, keepdims=True)
    inputs, cots, weights_all, decays = call(
        functools.partial(gather_kernel, groups),
        [
            ((groups * tok_rows, width), BF16),
            ((groups * tok_rows, width), BF16),
            ((groups, groups, tok_rows), F32),
            ((groups, 1, log_decay.shape[1]), F32),
        ],
        moe_input,
        cotangent,
        weights,
        decay_sum,
        sems=(4 * (groups - 1), 2 * (groups - 1)),
        ident=1,
    )
    mine = lax.dynamic_index_in_dim(weights_all, me, 1, keepdims=False).reshape(-1, 1)
    decays = decays[:, 0]

    gate_weight, up_weight, down_weight = w_gate[0], w_up[0], w_down[0]
    gate = jnp.dot(inputs, gate_weight, preferred_element_type=F32)
    upper = jnp.dot(inputs, up_weight, preferred_element_type=F32)
    routed = (mine * cots.astype(F32)).astype(BF16)
    sigmoid_gate = jax.nn.sigmoid(gate)
    active = gate * sigmoid_gate
    hidden = (active * upper).astype(BF16)
    d_hidden = dot(routed, down_weight, NT, None)
    d_upper = (d_hidden * active).astype(BF16)
    d_gate = (d_hidden * upper * sigmoid_gate * (1.0 + gate * (1.0 - sigmoid_gate))).astype(BF16)
    slots = (dot(d_gate, gate_weight, NT, None) + dot(d_upper, up_weight, NT, None)).astype(BF16)
    half, depth = tok_rows // 2, lanes // 2
    (grad_in,) = call(
        functools.partial(sum_kernel, groups),
        [((tok_rows, width), BF16)],
        slots,
        cotangent,
        scratch=[
            (groups, half, width),
            (groups, half, width),
            (groups - 1, half, width),
            (half, width),
            (depth - 1, half // depth, width),
        ],
        sems=(groups, groups - 1, depth - 1, depth - 1, 1),
        ident=2,
    )
    grad_gate, grad_up, grad_down = weight_grads(inputs, routed, hidden, d_gate, d_upper)

    channels, wide = queries.shape[1], span_state.shape[2]
    mix, starts = call(
        functools.partial(mix_kernel, groups),
        [((tok_rows, values.shape[1]), F32), ((groups, channels, wide), F32)],
        grad_in,
        out_proj,
        queries,
        log_decay,
        sems=(groups - 1,),
        ident=3,
    )
    grad_proj = lax.psum_scatter(
        dot(grad_in, saved_out, TN, None).astype(BF16), "sp", scatter_dimension=0, tiled=True
    ).astype(F32)
    at = jnp.arange(groups, dtype=jnp.int32)
    between = ((at[None, :] > me) & (at[None, :] < at[:, None])).astype(F32)
    factor = jnp.exp(jnp.sum(between[:, :, None] * decays[None], axis=1))
    factor = jnp.where((at > me)[:, None], factor, 0.0)
    after = jnp.sum(factor[:, :, None] * starts, axis=0)
    grad_queries, grad_keys, grad_values, grad_decay = call(
        finish_kernel,
        [
            (queries.shape, BF16),
            (keys.shape, BF16),
            (values.shape, BF16),
            (log_decay.shape, F32),
        ],
        queries,
        keys,
        values,
        log_decay,
        mix,
        span_state,
        after,
    )
    return (
        grad_gate,
        grad_up,
        grad_down,
        grad_proj,
        grad_queries,
        grad_keys,
        grad_values,
        grad_decay,
    )


def solution(mesh):
    placed = (
        P("sp", None),
        P("sp", None),
        P("sp", None),
        P("sp", None),
        P("sp", None, "tp"),
        P("sp", None, "tp"),
        P("sp", "tp", None),
        P("tp", None),
        P("sp", "tp"),
        P("sp", "tp"),
        P("sp", "tp"),
        P("sp", "tp"),
        P("sp", "tp"),
        P("sp", "tp", None),
    )
    return jax.shard_map(
        on_device,
        mesh=mesh,
        in_specs=placed,
        out_specs=(
            P("sp", None, "tp"),
            P("sp", None, "tp"),
            P("sp", "tp", None),
            P("sp", "tp"),
            P("sp", "tp"),
            P("sp", "tp"),
            P("sp", "tp"),
            P("sp", "tp"),
        ),
        check_vma=False,
    )
```
